1024 devices in a mesh: sp: 128 (over z, y), tp: 8 (over x, core).
Axes of the slice: x: 4, y: 8, z: 16, core: 2. Of those that a mesh axis runs over, the one named last changes fastest.
Arguments:
- tokens: bfloat16 [49152, 2048], P('sp'), may hold values from -6 to 6
- in_gain: float32 [2048], replicated, may hold values from 0.1 to 1.9
- query_weight: bfloat16 [2048, 1024], P(None, 'tp'), may hold values from -0.125 to 0.125
- key_weight: bfloat16 [2048, 1024], P(None, 'tp'), may hold values from -0.125 to 0.125
- value_weight: bfloat16 [2048, 2048], P(None, 'tp'), may hold values from -0.125 to 0.125
- gate_weight: bfloat16 [2048, 2048], P(None, 'tp'), may hold values from -0.125 to 0.125
- decay_down: bfloat16 [2048, 32], replicated, may hold values from -0.125 to 0.125
- decay_up: bfloat16 [32, 1024], replicated, may hold values from -1 to 1
- decay_offset: float32 [1024], P('tp')
- decay_extra: float32 [49152, 1024], P('sp', 'tp'), may hold values from -2 to 0, as said below
- head_gain: float32 [2048], P('tp'), may hold values from 0.1 to 1.9
- out_weight: bfloat16 [2048, 2048], P(None, 'tp'), may hold values from -4 to 4
- out_gain: float32 [2048], P('tp'), may hold values from 0.1 to 1.9
Outputs:
- layer_output: bfloat16 [49152, 2048], P('sp', 'tp')
The draws below stay inside these ranges and needn't reach their ends.
Inputs may be any that keep to these rules, and one draw needn't show every extreme that they name: `decay_extra`: never positive.
All inputs are finite; a program needn't handle non-finite values.
Results may differ from the reference program's by a relative error of at most 0.015.
Values may be sent and summed in bfloat16 or wider, within the bound.
A program may use at most 64 MiB of HBM per device.

```python
import math
import jax
import jax.numpy as jnp
from jax import lax

D = 2048
ATTENTION_UNITS = 8
QUERY_FEATURES = 128
DV = 256
RANK = 32
BLOCK = 64
TOK = 384
TOKEN_SPAN = 49152
KW = 1024
VW = 2048


def draw_decay_offset(key, part):
    base_key = jax.random.fold_in(key, 11)
    order_key, jitter_key = jax.random.split(base_key)
    jitter = jax.random.uniform(jitter_key, (ATTENTION_UNITS, QUERY_FEATURES), jnp.float32, -0.5, 0.5)
    slow_level = math.log(4.0 * TOKEN_SPAN / 16.0)
    ranking = jax.random.permutation(order_key, ATTENTION_UNITS)
    slow_heads = (ranking < ATTENTION_UNITS // 2)[:, None]
    levels = jnp.where(slow_heads, slow_level, 0.0) + jitter
    return levels.reshape(ATTENTION_UNITS * QUERY_FEATURES).astype(jnp.float32)


def draw_decay_extra(key, part):
    base_key = jax.random.fold_in(key, 23)
    rate_key, channel_key, place_key, depth_key = jax.random.split(base_key, 4)
    block_total = TOKEN_SPAN // TOK
    block_rates = jnp.exp(jax.random.uniform(rate_key, (block_total, 1, ATTENTION_UNITS, 1), jnp.float32, math.log(0.1), math.log(2.0)))
    channel_rates = jnp.exp(jax.random.uniform(channel_key, (1, 1, ATTENTION_UNITS, QUERY_FEATURES), jnp.float32, math.log(0.5), math.log(2.0)))
    constant_amount = jnp.broadcast_to(-(block_rates * channel_rates) / TOKEN_SPAN, (block_total, TOK, ATTENTION_UNITS, QUERY_FEATURES))
    location_cells = jax.random.randint(place_key, (2, ATTENTION_UNITS), 0, TOKEN_SPAN)
    layer_tiers = jax.random.uniform(depth_key, (2, ATTENTION_UNITS), jnp.float32, math.log(0.5), math.log(0.8))
    token_ordinal = jnp.arange(TOKEN_SPAN)[:, None, None]
    packet_clusters = jnp.sum(jnp.where(token_ordinal == location_cells[None], layer_tiers[None], 0.0), axis=1)
    overall_number = constant_amount.reshape(TOKEN_SPAN, ATTENTION_UNITS, QUERY_FEATURES) + packet_clusters[:, :, None]
    return overall_number.reshape(TOKEN_SPAN, ATTENTION_UNITS * QUERY_FEATURES).astype(jnp.float32)


def draw_out_weight(key, part):
    base_key = jax.random.fold_in(key, 37)
    weight_key, jitter_key = jax.random.split(base_key)
    values = jax.random.truncated_normal(weight_key, -4.0, 4.0, (VW, D), jnp.float32) / math.sqrt(VW)
    columns = jnp.arange(D).astype(jnp.float32) / D
    jitter = jax.random.uniform(jitter_key, (D,), jnp.float32, 0.0, 1.0)
    exponent = (columns + jitter / 8.0) / 1.125
    return (values * jnp.power(10.0, exponent)[None, :]).astype(jnp.bfloat16)


def steps_of(rng, extent, shards, smallest, largest):
    loudness, own = 1.0, jax.random.fold_in(rng, 6)
    for dim, shards_of in shards:
        draws = jnp.exp(jax.random.uniform(jax.random.fold_in(own, dim), (shards_of,), jnp.float32, smallest / len(shards), largest / len(shards)))
        loudness = loudness * jnp.repeat(draws, extent[dim] // shards_of).reshape([-1 if axis == dim else 1 for axis in range(len(extent))])
    return loudness


def bell_draw(rng, extent, spread, most, shards=(), dtype=jnp.bfloat16):
    factor_of = steps_of(rng, extent, shards, -0.22, 0.18) if shards else 1.0
    array = jax.random.normal(rng, extent, jnp.float32) * spread * factor_of
    return jnp.minimum(jnp.maximum(array, -most), most).astype(dtype)


def setup_inputs(seed: int = 0) -> dict:
    key_of = jax.random.split(jax.random.key(seed), 14)
    return {
        "tokens": bell_draw(key_of[0], (TOKEN_SPAN, D), 1.0, 6.0, ((0, 128),)),
        "in_gain": jnp.clip(1.0 + 0.18 * jax.random.normal(key_of[1], (D,), jnp.float32), 0.1, 1.9),
        "query_weight": bell_draw(key_of[2], (D, KW), D ** -0.5, 0.125, ((1, 8),)),
        "key_weight": bell_draw(key_of[3], (D, KW), D ** -0.5, 0.125, ((1, 8),)),
        "value_weight": bell_draw(key_of[4], (D, VW), D ** -0.5, 0.125, ((1, 8),)),
        "gate_weight": bell_draw(key_of[5], (D, VW), D ** -0.5, 0.125, ((1, 8),)),
        "decay_down": bell_draw(key_of[6], (D, RANK), D ** -0.5, 0.125),
        "decay_up": bell_draw(key_of[7], (RANK, KW), RANK ** -0.5, 1.0),
        "decay_offset": draw_decay_offset(jax.random.fold_in(key_of[13], 71), 0),
        "decay_extra": draw_decay_extra(jax.random.fold_in(key_of[13], 71), 0),
        "head_gain": jnp.clip(1.0 + 0.18 * jax.random.normal(key_of[10], (VW,), jnp.float32), 0.1, 1.9),
        "out_weight": draw_out_weight(jax.random.fold_in(key_of[13], 71), 0),
        "out_gain": jnp.clip(1.0 + 0.18 * jax.random.normal(key_of[12], (D,), jnp.float32), 0.1, 1.9),
    }


norm_eps = 1e-06
decay_temper = 16.0

def reference(tokens, in_gain, query_weight, key_weight, value_weight, gate_weight, decay_down, decay_up, decay_offset, decay_extra, head_gain, out_weight, out_gain):
    highest = lax.Precision.HIGHEST
    tokens_wide = tokens.astype(jnp.float32)
    normed = (tokens_wide * lax.rsqrt(lax.optimization_barrier(jnp.mean(tokens_wide * tokens_wide, axis=1, keepdims=True)) + norm_eps) * in_gain).astype(jnp.bfloat16)

    def project(weight):
        return jnp.dot(normed, weight, preferred_element_type=jnp.float32).astype(jnp.bfloat16)
    query_rows = project(query_weight)
    key_rows = project(key_weight)
    value_rows = project(value_weight)
    gate_rows = project(gate_weight)
    low_rank = project(decay_down)
    logits = jnp.dot(low_rank, decay_up, preferred_element_type=jnp.float32)
    log_decay = jax.nn.log_sigmoid(logits + decay_offset) / decay_temper + decay_extra
    block_count = TOKEN_SPAN // BLOCK

    def to_blocks(values, width):
        return values.astype(jnp.float32).reshape(block_count, BLOCK, ATTENTION_UNITS, width)
    causal_mask = jnp.arange(BLOCK)[:, None] >= jnp.arange(BLOCK)[None, :]

    def block_step(carry_state, inputs):
        query_block, key_block, value_block, decay_block = inputs
        cumulative = jnp.cumsum(decay_block, axis=0)
        closing = cumulative[-1]
        query_inner = query_block * jnp.exp(cumulative)
        key_inner = key_block * jnp.exp(-cumulative)
        scores = jnp.einsum('chd,shd->hcs', query_inner, key_inner, precision=highest)
        scores = jnp.where(causal_mask[None], scores, 0.0)
        output = jnp.einsum('hcs,she->che', scores, value_block, precision=highest)
        output = output + jnp.einsum('chd,hde->che', query_inner, carry_state, precision=highest)
        key_closing = key_block * jnp.exp(closing[None] - cumulative)
        carry_state = carry_state * jnp.exp(closing)[:, :, None] + jnp.einsum('chd,che->hde', key_closing, value_block, precision=highest)
        return (carry_state, output)
    start_state = jnp.zeros((ATTENTION_UNITS, QUERY_FEATURES, DV), jnp.float32)
    final_state, outputs = lax.scan(block_step, start_state, (to_blocks(query_rows, QUERY_FEATURES), to_blocks(key_rows, QUERY_FEATURES), to_blocks(value_rows, DV), to_blocks(log_decay, QUERY_FEATURES)))
    attended = outputs.reshape(TOKEN_SPAN, ATTENTION_UNITS, DV)
    scaled = attended * lax.rsqrt(lax.optimization_barrier(jnp.mean(attended * attended, axis=2, keepdims=True)) + norm_eps) * head_gain.reshape(ATTENTION_UNITS, DV)
    gated = (scaled.reshape(TOKEN_SPAN, ATTENTION_UNITS * DV) * jax.nn.silu(gate_rows.astype(jnp.float32))).astype(jnp.bfloat16)
    mixed = jnp.dot(gated, out_weight, preferred_element_type=jnp.float32)
    result = mixed * lax.rsqrt(lax.optimization_barrier(jnp.mean(mixed * mixed, axis=1, keepdims=True)) + norm_eps) * out_gain
    return result.astype(jnp.bfloat16)
```

```python
import functools

import jax
import jax.numpy as jnp
from jax import lax
from jax.experimental import pallas as pl
from jax.experimental.pallas import tpu as pltpu
from jax.sharding import Mesh
from jax.sharding import PartitionSpec as P

QUERY_FEATURES = 128
DV = 256
CHUNK = 128
NX = 4
norm_eps = 1e-06
decay_temper = 16.0
MESH = pl.DeviceIdType.MESH
f32 = jnp.float32
bf16 = jnp.bfloat16


def dot(a, b, ca=1, cb=0):
    return lax.dot_general(a, b, (((ca,), (cb,)), ((), ())), preferred_element_type=f32)


def dot_wide(a, b):
    a_hi, b_hi = a.astype(bf16), b.astype(bf16)
    a_lo, b_lo = (a - a_hi.astype(f32)).astype(bf16), (b - b_hi.astype(f32)).astype(bf16)
    return dot(jnp.concatenate([a_hi, a_hi, a_lo], axis=1), jnp.concatenate([b_hi, b_lo, b_hi], axis=1), 1, 1)


def far_first(n):
    return sorted(range(1, n), key=lambda o: -min(o, n - o))


def kernel(
    nz,
    ny,
    tok_h,
    ing_h,
    wq_h,
    wk_h,
    wv_h,
    wg_h,
    dd_h,
    du_h,
    off_h,
    ext_h,
    hg_h,
    wo_h,
    og_h,
    out_ref,
    tok,
    nrm,
    wq,
    wk,
    wv,
    wg,
    wo,
    dd,
    du,
    ing,
    doff,
    ext,
    hg,
    og,
    cum,
    kk,
    vv,
    qq,
    fac,
    qhat,
    att,
    st,
    gsend,
    arr,
    garr,
    inside,
    wbuf,
    tsend,
    gtsend,
    zarr,
    zgarr,
    bsend,
    sin,
    gat,
    acc,
    ssend,
    sarr,
    lsem,
    s1s,
    s1r,
    g1s,
    g1r,
    s2s,
    s2r,
    g2s,
    g2r,
    s3s,
    s3r,
    gs,
    gr,
    nss,
    nsr,
):
    z, y, x, c = (lax.axis_index(name) for name in ("z", "y", "x", "c"))
    rows, width = tok.shape
    half = rows // 2
    chunks = rows // CHUNK
    piece = DV // ny
    me = x * 2 + c
    plus, minus, across = lax.rem(x + 1, NX), lax.rem(x + NX - 1, NX), lax.rem(x + 2, NX)

    loads = []

    def load(src, dst):
        copy = pltpu.make_async_copy(src, dst, lsem.at[len(loads)])
        copy.start()
        loads.append(copy)
        return copy

    ld_tok = load(tok_h, tok)
    ld_ing = load(ing_h, ing)
    ld_dd = load(dd_h, dd)
    ld_du = load(du_h.at[:, pl.ds(pl.multiple_of(me * QUERY_FEATURES, QUERY_FEATURES), QUERY_FEATURES)], du)
    ld_off = load(off_h, doff)
    ld_ext = load(ext_h, ext)
    ld_wk = load(wk_h, wk)
    ld_wv = load(wv_h, wv)
    ld_wq = load(wq_h, wq)
    ld_wg = load(wg_h, wg)
    ld_hg = load(hg_h, hg)
    ld_wo = load(wo_h, wo)
    ld_og = load(og_h, og)

    barrier = pltpu.get_barrier_semaphore()
    peers = [{"y": lax.rem(y + o, ny)} for o in range(1, ny)]
    peers += [{"z": lax.rem(z + o, nz)} for o in range(1, nz)]
    tps = [(o, t) for o in range(NX) for t in range(2) if (o, t) != (0, 0)]
    tp_peers = [{"x": lax.rem(x + o, NX), "c": lax.rem(c + t, 2)} for o, t in tps]
    peers += tp_peers
    for peer in peers:
        pl.semaphore_signal(barrier, inc=1, device_id=peer, device_id_type=MESH)

    ld_tok.wait()
    ld_ing.wait()

    def norm_rows(i, carry):
        at = pl.ds(pl.multiple_of(i * 16, 16), 16)
        wide = tok[at, :].astype(f32)
        scale = lax.rsqrt(jnp.mean(wide * wide, axis=1, keepdims=True) + norm_eps)
        nrm[at, :] = (wide * scale * ing[...]).astype(bf16)
        return carry

    lax.fori_loop(0, rows // 16, norm_rows, 0, unroll=4)

    ld_dd.wait()
    ld_du.wait()
    ld_off.wait()
    ld_ext.wait()
    low = dot(nrm[...], dd[...]).astype(bf16)
    pre = dot(low, du[...]) + doff[...]
    log_decay = (jnp.minimum(pre, 0.0) - jnp.log1p(jnp.exp(-jnp.abs(pre)))) / decay_temper + ext[...]
    d_hi = log_decay.astype(bf16)
    rest = log_decay - d_hi.astype(f32)
    d_mid = rest.astype(bf16)
    d_low = (rest - d_mid.astype(f32)).astype(bf16)
    lower = lax.broadcasted_iota(jnp.int32, (rows, rows), 0) >= lax.broadcasted_iota(jnp.int32, (rows, rows), 1)
    lower = jnp.where(lower, 1.0, 0.0).astype(bf16)
    cum[...] = dot(lower, d_hi) + (dot(lower, d_mid) + dot(lower, d_low))
    closing = cum[rows - 1 : rows, :]
    gsend[...] = closing
    garr[y] = closing

    ld_wk.wait()
    ld_wv.wait()
    kk[...] = dot(nrm[...], wk[...]).astype(bf16)
    vv[...] = dot(nrm[...], wv[...]).astype(bf16)
    khat = (kk[...].astype(f32) * jnp.exp(closing - cum[...])).astype(bf16)
    state = dot(vv[...], khat, 0, 0).astype(bf16)
    st[...] = state.reshape(ny, piece, QUERY_FEATURES)
    arr[y] = st[y]

    pl.semaphore_wait(barrier, len(peers))

    def copy1(o):
        to = lax.rem(y + o, ny)
        return (
            pltpu.make_async_remote_copy(
                src_ref=st.at[to], dst_ref=arr.at[y], send_sem=s1s.at[o], recv_sem=s1r.at[o],
                device_id={"y": to}, device_id_type=MESH),
            pltpu.make_async_remote_copy(
                src_ref=gsend, dst_ref=garr.at[y], send_sem=g1s.at[o], recv_sem=g1r.at[o],
                device_id={"y": to}, device_id_type=MESH),
        )

    def got1(o):
        src = lax.rem(y + ny - o, ny)
        return (
            pltpu.make_async_remote_copy(
                src_ref=st.at[src], dst_ref=arr.at[src], send_sem=s1s.at[o], recv_sem=s1r.at[o],
                device_id={"y": src}, device_id_type=MESH),
            pltpu.make_async_remote_copy(
                src_ref=gsend, dst_ref=garr.at[src], send_sem=g1s.at[o], recv_sem=g1r.at[o],
                device_id={"y": src}, device_id_type=MESH),
        )

    for o in far_first(ny):
        for copy in copy1(o):
            copy.start()

    ld_wq.wait()
    qq[...] = dot(nrm[...], wq[...]).astype(bf16)
    qhat[...] = (qq[...].astype(f32) * jnp.exp(cum[...])).astype(bf16)
    ld_wg.wait()
    ld_hg.wait()
    gate = dot(nrm[...], wg[...]).astype(bf16).astype(f32)
    fac[...] = gate * (1.0 / (1.0 + jnp.exp(-gate))) * hg[...]

    for o in range(1, ny):
        for copy in got1(o):
            copy.wait_recv()
    run = jnp.zeros((piece, QUERY_FEATURES), f32)
    total = jnp.zeros((1, QUERY_FEATURES), f32)
    for k in range(ny):
        inside[k] = run
        wbuf[k] = jnp.exp(total)
        run = jnp.exp(garr[k]) * run + arr[k].astype(f32)
        total = total + garr[k]
    tsend[...] = run.astype(bf16)
    gtsend[...] = total

    def copy2(d):
        to = lax.rem(z + d, nz)
        return (
            pltpu.make_async_remote_copy(
                src_ref=tsend, dst_ref=zarr.at[d], send_sem=s2s.at[d], recv_sem=s2r.at[d],
                device_id={"z": to}, device_id_type=MESH),
            pltpu.make_async_remote_copy(
                src_ref=gtsend, dst_ref=zgarr.at[d], send_sem=g2s.at[d], recv_sem=g2r.at[d],
                device_id={"z": to}, device_id_type=MESH),
        )

    later = nz - 1 - z

    def send2(i, carry):
        for copy in copy2(later - i):
            copy.start()
        return carry

    lax.fori_loop(0, later, send2, 0)

    size = (CHUNK, CHUNK)
    r_at, c_at = lax.broadcasted_iota(jnp.int32, size, 0), lax.broadcasted_iota(jnp.int32, size, 1)
    mid = CHUNK // 2
    same = (r_at >= c_at) & ((r_at >= mid) == (c_at >= mid))
    cross = (r_at >= mid) & (c_at < mid)
    for i in range(chunks):
        lo = i * CHUNK
        own = slice(lo, lo + CHUNK)
        q = qq[own, :].astype(f32)
        k = kk[own, :].astype(f32)
        at = cum[own, :]
        pivot = jnp.concatenate(
            [jnp.broadcast_to(cum[lo + j + mid // 2 - 1 : lo + j + mid // 2, :], (mid, QUERY_FEATURES)) for j in (0, mid)], axis=0)
        border = cum[lo + mid - 1 : lo + mid, :]
        near = dot_wide(q * jnp.exp(at - pivot), k * jnp.exp(pivot - at))
        step = dot_wide(q * jnp.exp(jnp.minimum(at - border, 0.0)), k * jnp.exp(jnp.minimum(border - at, 0.0)))
        scores = jnp.where(same, near, jnp.where(cross, step, 0.0)).astype(bf16)
        result = dot(scores, vv[own, :])
        if i:
            start = cum[lo - 1 : lo, :]
            before = slice(0, lo)
            earlier = dot_wide(
                q * jnp.exp(at - start), kk[before, :].astype(f32) * jnp.exp(start - cum[before, :]))
            result = result + dot(earlier.astype(bf16), vv[before, :])
        att[own, :] = result

    def take2(d, carry):
        into, weight = carry
        for copy in copy2(d):
            copy.wait_recv()
        return into + jnp.exp(weight) * zarr[d].astype(f32), weight + zgarr[d]

    ahead, _ = lax.fori_loop(
        1, z + 1, take2,
        (jnp.zeros((piece, QUERY_FEATURES), f32), jnp.zeros((1, QUERY_FEATURES), f32)))

    for k in range(ny):
        bsend[k] = (wbuf[k] * ahead + inside[k]).astype(bf16)

    def copy3(o):
        to = lax.rem(y + o, ny)
        return pltpu.make_async_remote_copy(
            src_ref=bsend.at[to], dst_ref=sin.at[y], send_sem=s3s.at[o], recv_sem=s3r.at[o],
            device_id={"y": to}, device_id_type=MESH)

    def got3(o):
        src = lax.rem(y + ny - o, ny)
        return pltpu.make_async_remote_copy(
            src_ref=bsend.at[src], dst_ref=sin.at[src], send_sem=s3s.at[o], recv_sem=s3r.at[o],
            device_id={"y": src}, device_id_type=MESH)

    for o in far_first(ny):
        copy3(o).start()
    sin[y] = bsend[y]
    for o in range(1, ny):
        got3(o).wait_recv()
    come = sin[...].reshape(DV, QUERY_FEATURES)

    first, second = pl.ds(0, half), pl.ds(half, half)

    def go(slot, part, k, where):
        return pltpu.make_async_remote_copy(
            src_ref=gat.at[slot, part], dst_ref=gat.at[slot, part], send_sem=gs.at[k], recv_sem=gr.at[k],
            device_id=where, device_id_type=MESH)

    east, west, other = {"x": plus}, {"x": minus}, {"c": 1 - c}
    from_west, from_east, from_far = minus * 2 + c, plus * 2 + c, across * 2 + c
    twin = 1 - 2 * c

    for part, sends in ((first, ((0, east), (3, west), (6, other))), (second, ((2, west), (1, east), (7, other)))):
        there = att[part, :] + dot(qhat[part, :], come, 1, 1)
        scale = lax.rsqrt(jnp.mean(there * there, axis=1, keepdims=True) + norm_eps)
        gat[me, part, :] = (there * scale * fac[part, :]).astype(bf16)
        for k, where in sends:
            go(me, part, k, where).start()

    ld_wo.wait()

    def add(slot, part, fresh=False):
        term = dot(gat[slot, part, :], wo[pl.ds(pl.multiple_of(slot * DV, DV), DV), :])
        acc[part, :] = term if fresh else acc[part, :] + term

    add(me, first, True)
    add(me, second, True)
    go(from_west, first, 0, west).wait_recv()
    go(from_west, first, 4, east).start()
    go(from_west, first, 8, other).start()
    go(from_east, second, 2, east).wait_recv()
    go(from_east, second, 5, west).start()
    go(from_east, second, 9, other).start()
    go(me + twin, first, 6, other).wait_recv()
    go(me + twin, second, 7, other).wait_recv()
    add(me + twin, first)
    add(me + twin, second)
    add(from_west, first)
    add(from_east, second)
    go(from_west, second, 1, west).wait_recv()
    go(from_west, second, 10, other).start()
    go(from_east, first, 3, east).wait_recv()
    go(from_east, first, 11, other).start()
    add(from_west, second)
    add(from_east, first)
    go(from_west + twin, first, 8, other).wait_recv()
    add(from_west + twin, first)
    go(from_east + twin, second, 9, other).wait_recv()
    add(from_east + twin, second)
    go(from_west + twin, second, 10, other).wait_recv()
    add(from_west + twin, second)
    go(from_east + twin, first, 11, other).wait_recv()
    add(from_east + twin, first)
    go(from_far, first, 4, west).wait_recv()
    go(from_far, first, 12, other).start()
    go(from_far, second, 5, east).wait_recv()
    go(from_far, second, 13, other).start()
    add(from_far, first)
    add(from_far, second)
    go(from_far + twin, first, 12, other).wait_recv()
    add(from_far + twin, first)
    go(from_far + twin, second, 13, other).wait_recv()
    add(from_far + twin, second)

    mixed = acc[...]
    folded = mixed * mixed
    folded = folded[:, :128] + folded[:, 128:]
    ssend[...] = jnp.zeros_like(ssend)
    for i in range(chunks):
        flipped = folded[i * CHUNK : (i + 1) * CHUNK, :].T
        ssend[i : i + 1, :] = jnp.sum(flipped, axis=0, keepdims=True)

    def copy_ss(j):
        return pltpu.make_async_remote_copy(
            src_ref=ssend, dst_ref=sarr.at[me], send_sem=nss.at[j], recv_sem=nsr.at[j],
            device_id=tp_peers[j], device_id_type=MESH)

    def got_ss(j):
        o, t = tps[j]
        src_x, src_c = lax.rem(x + NX - o, NX), lax.rem(c + t, 2)
        return pltpu.make_async_remote_copy(
            src_ref=ssend, dst_ref=sarr.at[src_x * 2 + src_c], send_sem=nss.at[j], recv_sem=nsr.at[j],
            device_id={"x": src_x, "c": src_c}, device_id_type=MESH)

    for j in range(len(tps)):
        copy_ss(j).start()
    sarr[me] = ssend[...]
    ld_og.wait()
    for j in range(len(tps)):
        got_ss(j).wait_recv()
    squares = sarr[0]
    for j in range(1, 2 * NX):
        squares = squares + sarr[j]
    inverse = lax.rsqrt(squares / (2 * NX * DV) + norm_eps)
    for i in range(chunks):
        own = slice(i * CHUNK, (i + 1) * CHUNK)
        per_row = jnp.broadcast_to(inverse[i : i + 1, :], size).T
        for j in range(0, DV, 128):
            out_ref[own, j : j + 128] = (acc[own, j : j + 128] * per_row * og[:, j : j + 128]).astype(out_ref.dtype)

    for o in range(1, ny):
        for copy in copy1(o):
            copy.wait_send()
        copy3(o).wait_send()

    def sent2(i, carry):
        for copy in copy2(later - i):
            copy.wait_send()
        return carry

    lax.fori_loop(0, later, sent2, 0)
    for k, part in enumerate((first, second, second, first, first, second, first, second,
                              first, second, second, first, first, second)):
        go(me, part, k, other).wait_send()
    for j in range(len(tps)):
        copy_ss(j).wait_send()


def local(nz, ny, *args):
    (tokens, in_gain, query_weight, key_weight, value_weight, gate_weight, decay_down, decay_up,
     decay_offset, decay_extra, head_gain, out_weight, out_gain) = args
    rows, width = tokens.shape
    piece = DV // ny
    rank = decay_down.shape[1]
    in_hbm = pl.BlockSpec(memory_space=pltpu.HBM)
    dma = pltpu.SemaphoreType.DMA
    V = pltpu.VMEM
    scratch = [
        V((rows, width), bf16),
        V((rows, width), bf16),
        V((width, QUERY_FEATURES), bf16),
        V((width, QUERY_FEATURES), bf16),
        V((width, DV), bf16),
        V((width, DV), bf16),
        V((2 * NX * DV, DV), bf16),
        V((width, rank), bf16),
        V((rank, QUERY_FEATURES), bf16),
        V((1, width), f32),
        V((1, QUERY_FEATURES), f32),
        V((rows, QUERY_FEATURES), f32),
        V((1, DV), f32),
        V((1, DV), f32),
        V((rows, QUERY_FEATURES), f32),
        V((rows, QUERY_FEATURES), bf16),
        V((rows, DV), bf16),
        V((rows, QUERY_FEATURES), bf16),
        V((rows, DV), f32),
        V((rows, QUERY_FEATURES), bf16),
        V((rows, DV), f32),
        V((ny, piece, QUERY_FEATURES), bf16),
        V((1, QUERY_FEATURES), f32),
        V((ny, piece, QUERY_FEATURES), bf16),
        V((ny, 1, QUERY_FEATURES), f32),
        V((ny, piece, QUERY_FEATURES), f32),
        V((ny, 1, QUERY_FEATURES), f32),
        V((piece, QUERY_FEATURES), bf16),
        V((1, QUERY_FEATURES), f32),
        V((nz, piece, QUERY_FEATURES), bf16),
        V((nz, 1, QUERY_FEATURES), f32),
        V((ny, piece, QUERY_FEATURES), bf16),
        V((ny, piece, QUERY_FEATURES), bf16),
        V((2 * NX, rows, DV), bf16),
        V((rows, DV), f32),
        V((8, 128), f32),
        V((2 * NX, 8, 128), f32),
        dma((13,)),
        dma((ny,)), dma((ny,)), dma((ny,)), dma((ny,)),
        dma((nz,)), dma((nz,)), dma((nz,)), dma((nz,)),
        dma((ny,)), dma((ny,)),
        dma((14,)), dma((14,)),
        dma((2 * NX - 1,)), dma((2 * NX - 1,)),
    ]
    return pl.pallas_call(
        functools.partial(kernel, nz, ny),
        out_shape=jax.ShapeDtypeStruct((rows, DV), bf16),
        in_specs=[in_hbm] * 13,
        out_specs=pl.BlockSpec(memory_space=pltpu.VMEM),
        scratch_shapes=scratch,
        compiler_params=pltpu.CompilerParams(collective_id=0, has_side_effects=True, vmem_limit_bytes=48 << 20),
        name="linear_attention",
    )(
        tokens, in_gain.reshape(1, -1), query_weight, key_weight, value_weight, gate_weight, decay_down, decay_up,
        decay_offset.reshape(1, -1), decay_extra, head_gain.reshape(1, -1), out_weight, out_gain.reshape(1, -1),
    )


def build(devices, nz, ny):
    torus = Mesh(devices.reshape(nz, ny, NX, 2), ("z", "y", "x", "c"))
    sp, tp = ("z", "y"), ("x", "c")
    in_specs = (
        P(sp, None), P(), P(None, tp), P(None, tp), P(None, tp), P(None, tp), P(), P(), P(tp),
        P(sp, tp), P(tp), P(None, tp), P(tp),
    )
    return jax.shard_map(
        functools.partial(local, nz, ny), mesh=torus, in_specs=in_specs, out_specs=P(sp, tp), check_vma=False)


def solution(mesh):
    ny = 8
    return build(mesh.devices, mesh.shape["sp"] // ny, ny)
```

```python
import functools

import jax
import jax.numpy as jnp
from jax import lax
from jax.experimental import pallas as pl
from jax.experimental.pallas import tpu as pltpu
from jax.sharding import Mesh
from jax.sharding import PartitionSpec as P

QUERY_FEATURES = 128
DV = 256
CHUNK = 128
TOKEN_PARTS = 4
GROUP = 4
NX = 4
norm_eps = 1e-06
decay_temper = 16.0
MESH = pl.DeviceIdType.MESH
f32 = jnp.float32
bf16 = jnp.bfloat16


def dot(a, b, ca=1, cb=0):
    return lax.dot_general(a, b, (((ca,), (cb,)), ((), ())), preferred_element_type=f32)


def dot_wide(a, b):
    a_hi, b_hi = a.astype(bf16), b.astype(bf16)
    a_lo, b_lo = (a - a_hi.astype(f32)).astype(bf16), (b - b_hi.astype(f32)).astype(bf16)
    return dot(jnp.concatenate([a_hi, a_hi, a_lo], axis=1), jnp.concatenate([b_hi, b_lo, b_hi], axis=1), 1, 1)


def far_first(n):
    return sorted(range(1, n), key=lambda o: -min(o, n - o))


def kernel(
    nz,
    ny,
    tok_h,
    ing_h,
    wq_h,
    wk_h,
    wv_h,
    wg_h,
    dd_h,
    du_h,
    off_h,
    ext_h,
    hg_h,
    wo_h,
    og_h,
    out_ref,
    tok,
    nrm,
    wq,
    wk,
    wv,
    wg,
    wo,
    dd,
    du,
    ing,
    doff,
    ext,
    hg,
    og,
    cum,
    kk,
    vv,
    qq,
    fac,
    qhat,
    att,
    st,
    gsend,
    arr,
    garr,
    inside,
    wbuf,
    tsend,
    gtsend,
    zarr,
    zgarr,
    zfar,
    zgfar,
    bsend,
    sin,
    gat,
    acc,
    ssend,
    sarr,
    ready,
    lsem,
    s1s,
    s1r,
    g1s,
    g1r,
    s2s,
    s2r,
    g2s,
    g2r,
    s2f,
    g2f,
    s3s,
    s3r,
    gs,
    gr,
    nss,
    nsr,
):
    z, y, x, c = (lax.axis_index(name) for name in ("z", "y", "x", "c"))
    rows, width = tok.shape
    half = rows // 2
    chunks = rows // CHUNK
    piece = DV // ny
    me = x * 2 + c
    plus, minus, across = lax.rem(x + 1, NX), lax.rem(x + NX - 1, NX), lax.rem(x + 2, NX)

    loads = []

    def load(src, dst):
        copy = pltpu.make_async_copy(src, dst, lsem.at[len(loads)])
        copy.start()
        loads.append(copy)
        return copy

    ld_ing = load(ing_h, ing)
    part_rows = rows // TOKEN_PARTS
    ld_tok = [load(tok_h.at[pl.ds(i * part_rows, part_rows)], tok.at[pl.ds(i * part_rows, part_rows)]) for i in range(TOKEN_PARTS)]
    ld_dd = load(dd_h, dd)
    ld_du = load(du_h.at[:, pl.ds(pl.multiple_of(me * QUERY_FEATURES, QUERY_FEATURES), QUERY_FEATURES)], du)
    ld_off = load(off_h, doff)
    ld_ext = load(ext_h, ext)
    ld_wk = load(wk_h, wk)
    ld_wv = load(wv_h, wv)
    ld_wq = load(wq_h, wq)
    ld_wg = load(wg_h, wg)
    ld_hg = load(hg_h, hg)
    ld_wo = load(wo_h, wo)
    ld_og = load(og_h, og)

    barrier = pltpu.get_barrier_semaphore()
    peers = [{"y": lax.rem(y + o, ny)} for o in range(1, ny)]
    tps = [(o, t) for o in range(NX) for t in range(2) if (o, t) != (0, 0)]
    tp_peers = [{"x": lax.rem(x + o, NX), "c": lax.rem(c + t, 2)} for o, t in tps]
    peers += tp_peers
    for peer in peers:
        pl.semaphore_signal(barrier, inc=1, device_id=peer, device_id_type=MESH)
    later = nz - 1 - z
    group, place = lax.div(z, GROUP), lax.rem(z, GROUP)
    last = place == GROUP - 1
    reach = jnp.where(last, later, GROUP - 1 - place)

    def greet(d, carry):
        pl.semaphore_signal(barrier, inc=1, device_id={"z": z + d}, device_id_type=MESH)
        return carry

    lax.fori_loop(1, reach + 1, greet, 0)

    ld_ing.wait()

    def norm_rows(i, carry):
        at = pl.ds(pl.multiple_of(i * 16, 16), 16)
        wide = tok[at, :].astype(f32)
        scale = lax.rsqrt(jnp.mean(wide * wide, axis=1, keepdims=True) + norm_eps)
        nrm[at, :] = (wide * scale * ing[...]).astype(bf16)
        return carry

    tiles = part_rows // 16
    for i in range(TOKEN_PARTS):
        ld_tok[i].wait()
        lax.fori_loop(i * tiles, (i + 1) * tiles, norm_rows, 0, unroll=3)

    ld_dd.wait()
    ld_du.wait()
    ld_off.wait()
    ld_ext.wait()
    ld_wk.wait()
    ld_wv.wait()
    low = dot(nrm[...], dd[...], 1, 1).astype(bf16)
    pre = dot(low, du[...]) + doff[...]
    log_decay = (jnp.minimum(pre, 0.0) - jnp.log1p(jnp.exp(-jnp.abs(pre)))) / decay_temper + ext[...]
    d_hi = log_decay.astype(bf16)
    rest = log_decay - d_hi.astype(f32)
    d_mid = rest.astype(bf16)
    d_low = (rest - d_mid.astype(f32)).astype(bf16)
    lower = lax.broadcasted_iota(jnp.int32, (rows, rows), 0) >= lax.broadcasted_iota(jnp.int32, (rows, rows), 1)
    lower = jnp.where(lower, 1.0, 0.0).astype(bf16)
    cum[...] = dot(lower, d_hi) + (dot(lower, d_mid) + dot(lower, d_low))
    closing = cum[rows - 1 : rows, :]
    gsend[...] = closing
    garr[y] = closing

    kk[...] = dot(nrm[...], wk[...]).astype(bf16)
    vv[...] = dot(nrm[...], wv[...]).astype(bf16)
    khat = (kk[...].astype(f32) * jnp.exp(closing - cum[...])).astype(bf16)
    state = dot(vv[...], khat, 0, 0).astype(bf16)
    st[...] = state.reshape(ny, piece, QUERY_FEATURES)
    arr[y] = st[y]

    def copy1(o):
        to = lax.rem(y + o, ny)
        return (
            pltpu.make_async_remote_copy(
                src_ref=st.at[to], dst_ref=arr.at[y], send_sem=s1s, recv_sem=s1r,
                device_id={"y": to}, device_id_type=MESH),
            pltpu.make_async_remote_copy(
                src_ref=gsend, dst_ref=garr.at[y], send_sem=g1s, recv_sem=g1r,
                device_id={"y": to}, device_id_type=MESH),
        )

    def all_of(ref, count, sem):
        some = ref.at[pl.ds(0, count)]
        pltpu.make_async_copy(some, some, sem).wait()

    pl.semaphore_wait(barrier, len(peers) + place + group)
    for o in far_first(ny):
        for copy in copy1(o):
            copy.start()

    def tell_near(d, carry):
        pl.semaphore_signal(ready, inc=1, device_id={"z": z - d}, device_id_type=MESH)
        return carry

    def tell_last(g, carry):
        pl.semaphore_signal(ready, inc=1, device_id={"z": g * GROUP + GROUP - 1}, device_id_type=MESH)
        return carry

    lax.fori_loop(1, place + 1, tell_near, 0)
    lax.fori_loop(0, group, tell_last, 0)

    ld_wq.wait()
    qq[...] = dot(nrm[...], wq[...]).astype(bf16)
    qhat[...] = (qq[...].astype(f32) * jnp.exp(cum[...])).astype(bf16)
    ld_wg.wait()
    ld_hg.wait()
    gate = dot(nrm[...], wg[...]).astype(bf16).astype(f32)
    fac[...] = gate * (1.0 / (1.0 + jnp.exp(-gate))) * hg[...]

    size = (CHUNK, CHUNK)
    r_at, c_at = lax.broadcasted_iota(jnp.int32, size, 0), lax.broadcasted_iota(jnp.int32, size, 1)
    mid = CHUNK // 2
    same = (r_at >= c_at) & ((r_at >= mid) == (c_at >= mid))
    cross = (r_at >= mid) & (c_at < mid)
    for i in range(chunks):
        lo = i * CHUNK
        own = slice(lo, lo + CHUNK)
        q = qq[own, :].astype(f32)
        k = kk[own, :].astype(f32)
        at = cum[own, :]
        pivot = jnp.concatenate(
            [jnp.broadcast_to(cum[lo + j + mid // 2 - 1 : lo + j + mid // 2, :], (mid, QUERY_FEATURES)) for j in (0, mid)], axis=0)
        border = cum[lo + mid - 1 : lo + mid, :]
        near = dot_wide(q * jnp.exp(at - pivot), k * jnp.exp(pivot - at))
        step = dot_wide(q * jnp.exp(jnp.minimum(at - border, 0.0)), k * jnp.exp(jnp.minimum(border - at, 0.0)))
        scores = jnp.where(same, near, jnp.where(cross, step, 0.0)).astype(bf16)
        result = dot(scores, vv[own, :])
        if i:
            start = cum[lo - 1 : lo, :]
            before = slice(0, lo)
            earlier = dot_wide(
                q * jnp.exp(at - start), kk[before, :].astype(f32) * jnp.exp(start - cum[before, :]))
            result = result + dot(earlier.astype(bf16), vv[before, :])
        att[own, :] = result

    all_of(arr, ny - 1, s1r)
    all_of(garr, ny - 1, g1r)
    run = jnp.zeros((piece, QUERY_FEATURES), f32)
    total = jnp.zeros((1, QUERY_FEATURES), f32)
    for k in range(ny):
        inside[k] = run
        wbuf[k] = jnp.exp(total)
        run = jnp.exp(garr[k]) * run + arr[k].astype(f32)
        total = total + garr[k]
    tsend[0] = run.astype(bf16)
    gtsend[0] = total

    def copy2(level, d, slot, recv):
        send, land = (s2s, g2s), ((zarr, zgarr), (zfar, zgfar))[level]
        to = {"z": lax.rem(z + d, nz)}
        return [
            pltpu.make_async_remote_copy(
                src_ref=src.at[level], dst_ref=dst.at[slot], send_sem=sem.at[level], recv_sem=got.at[slot],
                device_id=to, device_id_type=MESH)
            for src, dst, sem, got in zip((tsend, gtsend), land, send, recv)
        ]

    @pl.when(reach > 0)
    def _():
        pl.semaphore_wait(ready, reach)

    def send_near(i, carry):
        d = GROUP - 1 - place - i
        for copy in copy2(0, d, d, (s2r, g2r)):
            copy.start()
        return carry

    lax.fori_loop(0, GROUP - 1 - place, send_near, 0)

    def take_near(d, carry):
        into, weight = carry
        for copy in copy2(0, d, d, (s2r, g2r)):
            copy.wait_recv()
        return into + jnp.exp(weight) * zarr[d].astype(f32), weight + zgarr[d]

    nothing = (jnp.zeros((piece, QUERY_FEATURES), f32), jnp.zeros((1, QUERY_FEATURES), f32))
    near, near_weight = lax.fori_loop(1, place + 1, take_near, nothing)

    @pl.when(last)
    def _():
        tsend[1] = (jnp.exp(total) * near + run).astype(bf16)
        gtsend[1] = near_weight + total

        def send_far(d, carry):
            for copy in copy2(1, d, group, (s2f, g2f)):
                copy.start()
            return carry

        lax.fori_loop(1, later + 1, send_far, 0)

    def take_far(i, carry):
        into, weight = carry
        g = group - 1 - i
        for copy in copy2(1, 1, g, (s2f, g2f)):
            copy.wait_recv()
        return into + jnp.exp(weight) * zfar[g].astype(f32), weight + zgfar[g]

    far, _ = lax.fori_loop(0, group, take_far, nothing)
    ahead = jnp.exp(near_weight) * far + near

    for k in range(ny):
        bsend[k] = (wbuf[k] * ahead + inside[k]).astype(bf16)

    first_of_all = (z == 0) & (y == 0)

    def copy3(o):
        to = lax.rem(y + o, ny)
        slot = y + jnp.where((z == 0) & (to == 0), ny, 0)
        return pltpu.make_async_remote_copy(
            src_ref=bsend.at[to], dst_ref=sin.at[slot], send_sem=s3s, recv_sem=s3r,
            device_id={"y": to}, device_id_type=MESH)

    for o in far_first(ny):
        copy3(o).start()

    @pl.when(first_of_all)
    def _():
        sin[pl.ds(0, ny)] = jnp.zeros((ny, piece, QUERY_FEATURES), bf16)

    @pl.when(jnp.logical_not(first_of_all))
    def _():
        sin[y] = bsend[y]
        all_of(sin, ny - 1, s3r)

    come = sin[pl.ds(0, ny)].reshape(DV, QUERY_FEATURES)

    first, second = pl.ds(0, half), pl.ds(half, half)

    def go(slot, part, k, where):
        return pltpu.make_async_remote_copy(
            src_ref=gat.at[slot, part], dst_ref=gat.at[slot, part], send_sem=gs, recv_sem=gr.at[k],
            device_id=where, device_id_type=MESH)

    east, west, other = {"x": plus}, {"x": minus}, {"c": 1 - c}
    from_west, from_east, from_far = minus * 2 + c, plus * 2 + c, across * 2 + c
    twin = 1 - 2 * c

    for part, sends in ((first, ((0, east), (6, other))), (second, ((2, west), (7, other)))):
        there = att[part, :] + dot(qhat[part, :], come, 1, 1)
        scale = lax.rsqrt(jnp.mean(there * there, axis=1, keepdims=True) + norm_eps)
        gat[me, part, :] = (there * scale * fac[part, :]).astype(bf16)
        for k, where in sends:
            go(me, part, k, where).start()
    go(me, second, 1, east).start()
    go(me, first, 3, west).start()

    ld_wo.wait()

    def add(slot, part, fresh=False):
        term = dot(gat[slot, part, :], wo[pl.ds(pl.multiple_of(slot * DV, DV), DV), :])
        acc[part, :] = term if fresh else acc[part, :] + term

    add(me, first, True)
    add(me, second, True)
    go(from_west, first, 0, west).wait_recv()
    go(from_west, first, 4, east).start()
    go(from_west, first, 8, other).start()
    go(from_east, second, 2, east).wait_recv()
    go(from_east, second, 5, west).start()
    go(from_east, second, 9, other).start()
    go(me + twin, first, 6, other).wait_recv()
    go(me + twin, second, 7, other).wait_recv()
    add(me + twin, first)
    add(me + twin, second)
    add(from_west, first)
    add(from_east, second)
    go(from_west, second, 1, west).wait_recv()
    go(from_west, second, 10, other).start()
    go(from_east, first, 3, east).wait_recv()
    go(from_east, first, 11, other).start()
    add(from_west, second)
    add(from_east, first)
    go(from_west + twin, first, 8, other).wait_recv()
    add(from_west + twin, first)
    go(from_east + twin, second, 9, other).wait_recv()
    add(from_east + twin, second)
    go(from_west + twin, second, 10, other).wait_recv()
    add(from_west + twin, second)
    go(from_east + twin, first, 11, other).wait_recv()
    add(from_east + twin, first)
    go(from_far, first, 4, west).wait_recv()
    go(from_far, first, 12, other).start()
    go(from_far, second, 5, east).wait_recv()
    go(from_far, second, 13, other).start()
    add(from_far, first)
    add(from_far, second)
    go(from_far + twin, first, 12, other).wait_recv()
    add(from_far + twin, first)
    go(from_far + twin, second, 13, other).wait_recv()
    add(from_far + twin, second)

    mixed = acc[...]
    folded = mixed * mixed
    folded = folded[:, :128] + folded[:, 128:]
    ssend[...] = jnp.zeros_like(ssend)
    for i in range(chunks):
        flipped = folded[i * CHUNK : (i + 1) * CHUNK, :].T
        ssend[i : i + 1, :] = jnp.sum(flipped, axis=0, keepdims=True)

    def copy_ss(j):
        return pltpu.make_async_remote_copy(
            src_ref=ssend, dst_ref=sarr.at[me], send_sem=nss, recv_sem=nsr,
            device_id=tp_peers[j], device_id_type=MESH)

    for j in range(len(tps)):
        copy_ss(j).start()
    sarr[me] = ssend[...]
    ld_og.wait()
    all_of(sarr, len(tps), nsr)
    squares = sarr[0]
    for j in range(1, 2 * NX):
        squares = squares + sarr[j]
    inverse = lax.rsqrt(squares / (2 * NX * DV) + norm_eps)
    for i in range(chunks):
        own = slice(i * CHUNK, (i + 1) * CHUNK)
        per_row = jnp.broadcast_to(inverse[i : i + 1, :], size).T
        for j in range(0, DV, 128):
            out_ref[own, j : j + 128] = (acc[own, j : j + 128] * per_row * og[:, j : j + 128]).astype(out_ref.dtype)

    @pl.when(first_of_all)
    def _():
        all_of(sin, ny - 1, s3r)

    all_of(st, ny - 1, s1s)
    all_of(garr, ny - 1, g1s)
    all_of(bsend, ny - 1, s3s)
    all_of(sarr, len(tps), nss)

    for p in range(GROUP - 1):
        @pl.when(place == p)
        def _(count=GROUP - 1 - p):
            all_of(zfar, count, s2s.at[0])
            all_of(zgfar, count, g2s.at[0])

    for g in range(nz // GROUP - 1):
        @pl.when(last & (group == g))
        def _(count=nz - GROUP * (g + 1)):
            all_of(zfar, count, s2s.at[1])
            all_of(zgfar, count, g2s.at[1])

    all_of(gat, 7, gs)


def local(nz, ny, *args):
    (tokens, in_gain, query_weight, key_weight, value_weight, gate_weight, decay_down, decay_up,
     decay_offset, decay_extra, head_gain, out_weight, out_gain) = args
    rows, width = tokens.shape
    piece = DV // ny
    rank = decay_down.shape[1]
    in_hbm = pl.BlockSpec(memory_space=pltpu.HBM)
    dma = pltpu.SemaphoreType.DMA
    V = pltpu.VMEM
    scratch = [
        V((rows, width), bf16),
        V((rows, width), bf16),
        V((width, QUERY_FEATURES), bf16),
        V((width, QUERY_FEATURES), bf16),
        V((width, DV), bf16),
        V((width, DV), bf16),
        V((2 * NX * DV, DV), bf16),
        V((rank, width), bf16),
        V((rank, QUERY_FEATURES), bf16),
        V((1, width), f32),
        V((1, QUERY_FEATURES), f32),
        V((rows, QUERY_FEATURES), f32),
        V((1, DV), f32),
        V((1, DV), f32),
        V((rows, QUERY_FEATURES), f32),
        V((rows, QUERY_FEATURES), bf16),
        V((rows, DV), bf16),
        V((rows, QUERY_FEATURES), bf16),
        V((rows, DV), f32),
        V((rows, QUERY_FEATURES), bf16),
        V((rows, DV), f32),
        V((ny, piece, QUERY_FEATURES), bf16),
        V((1, QUERY_FEATURES), f32),
        V((ny, piece, QUERY_FEATURES), bf16),
        V((ny, 1, QUERY_FEATURES), f32),
        V((ny, piece, QUERY_FEATURES), f32),
        V((ny, 1, QUERY_FEATURES), f32),
        V((2, piece, QUERY_FEATURES), bf16),
        V((2, 1, QUERY_FEATURES), f32),
        V((GROUP, piece, QUERY_FEATURES), bf16),
        V((GROUP, 1, QUERY_FEATURES), f32),
        V((nz, piece, QUERY_FEATURES), bf16),
        V((nz, 1, QUERY_FEATURES), f32),
        V((ny, piece, QUERY_FEATURES), bf16),
        V((2 * ny, piece, QUERY_FEATURES), bf16),
        V((2 * NX, rows, DV), bf16),
        V((rows, DV), f32),
        V((8, 128), f32),
        V((2 * NX, 8, 128), f32),
        pltpu.SemaphoreType.REGULAR,
        dma((12 + TOKEN_PARTS,)),
        dma, dma, dma, dma,
        dma((2,)), dma((GROUP,)), dma((2,)), dma((GROUP,)), dma((nz // GROUP,)), dma((nz // GROUP,)),
        dma, dma,
        dma, dma((14,)),
        dma, dma,
    ]
    operands = (
        tokens, in_gain.reshape(1, -1), query_weight, key_weight, value_weight, gate_weight, decay_down.T, decay_up,
        decay_offset.reshape(1, -1), decay_extra, head_gain.reshape(1, -1), out_weight, out_gain.reshape(1, -1),
    )
    return pl.pallas_call(
        functools.partial(kernel, nz, ny),
        out_shape=jax.ShapeDtypeStruct((rows, DV), bf16),
        in_specs=[in_hbm] * 13,
        out_specs=pl.BlockSpec(memory_space=pltpu.VMEM),
        scratch_shapes=scratch,
        compiler_params=pltpu.CompilerParams(collective_id=0, has_side_effects=True, vmem_limit_bytes=48 << 20),
        name="linear_attention",
    )(*(pltpu.with_memory_space_constraint(operand, pltpu.HBM) for operand in operands))


def build(devices, nz, ny):
    torus = Mesh(devices.reshape(nz, ny, NX, 2), ("z", "y", "x", "c"))
    sp, tp = ("z", "y"), ("x", "c")
    in_specs = (
        P(sp, None), P(), P(None, tp), P(None, tp), P(None, tp), P(None, tp), P(), P(), P(tp),
        P(sp, tp), P(tp), P(None, tp), P(tp),
    )
    return jax.shard_map(
        functools.partial(local, nz, ny), mesh=torus, in_specs=in_specs, out_specs=P(sp, tp), check_vma=False)


def solution(mesh):
    ny = 8
    return build(mesh.devices, mesh.shape["sp"] // ny, ny)
```

```python
import functools

import jax
import jax.numpy as jnp
from jax import lax
from jax.experimental import pallas as pl
from jax.experimental.pallas import tpu as pltpu
from jax.sharding import Mesh
from jax.sharding import PartitionSpec as P

QUERY_FEATURES = 128
DV = 256
CHUNK = 128
TOKEN_PARTS = 4
GROUP = 4
NX = 4
norm_eps = 1e-06
decay_temper = 16.0
MESH = pl.DeviceIdType.MESH
f32 = jnp.float32
bf16 = jnp.bfloat16


def dot(a, b, ca=1, cb=0):
    return lax.dot_general(a, b, (((ca,), (cb,)), ((), ())), preferred_element_type=f32)


def dot_wide(a, b):
    a_hi, b_hi = a.astype(bf16), b.astype(bf16)
    a_lo, b_lo = (a - a_hi.astype(f32)).astype(bf16), (b - b_hi.astype(f32)).astype(bf16)
    return dot(jnp.concatenate([a_hi, a_hi, a_lo], axis=1), jnp.concatenate([b_hi, b_lo, b_hi], axis=1), 1, 1)


def far_first(n):
    return sorted(range(1, n), key=lambda o: -min(o, n - o))


def kernel(
    nz,
    ny,
    tok_h,
    ing_h,
    wq_h,
    wk_h,
    wv_h,
    wg_h,
    dd_h,
    du_h,
    off_h,
    ext_h,
    hg_h,
    wo_h,
    og_h,
    out_ref,
    tok,
    nrm,
    wq,
    wk,
    wv,
    wg,
    wo,
    dd,
    du,
    ing,
    doff,
    ext,
    hg,
    og,
    cum,
    kk,
    vv,
    qq,
    fac,
    qhat,
    att,
    st,
    gsend,
    arr,
    garr,
    inside,
    wbuf,
    tsend,
    gtsend,
    zarr,
    zgarr,
    zfar,
    zgfar,
    bsend,
    sin,
    gat,
    acc,
    ssend,
    sarr,
    ready,
    lsem,
    s1s,
    s1r,
    g1s,
    g1r,
    s2s,
    s2r,
    g2s,
    g2r,
    s2f,
    g2f,
    s3s,
    s3r,
    gs,
    gr,
    nss,
    nsr,
):
    z, y, x, c = (lax.axis_index(name) for name in ("z", "y", "x", "c"))
    rows, width = tok.shape
    half = rows // 2
    chunks = rows // CHUNK
    piece = DV // ny
    me = x * 2 + c
    plus, minus, across = lax.rem(x + 1, NX), lax.rem(x + NX - 1, NX), lax.rem(x + 2, NX)

    loads = []

    def load(src, dst):
        copy = pltpu.make_async_copy(src, dst, lsem.at[len(loads)])
        copy.start()
        loads.append(copy)
        return copy

    part_rows = rows // TOKEN_PARTS
    ld_tok = [
        load(tok_h.at[pl.ds(i * part_rows, part_rows)], tok.at[pl.ds(i * part_rows, part_rows)])
        for i in range(TOKEN_PARTS)
    ]
    ld_ing = load(ing_h, ing)
    ld_dd = load(dd_h, dd)
    ld_du = load(du_h.at[:, pl.ds(pl.multiple_of(me * QUERY_FEATURES, QUERY_FEATURES), QUERY_FEATURES)], du)
    ld_off = load(off_h, doff)
    ld_ext = load(ext_h, ext)
    ld_wk = load(wk_h, wk)
    ld_wv = load(wv_h, wv)
    ld_wq = load(wq_h, wq)
    ld_wg = load(wg_h, wg)
    ld_hg = load(hg_h, hg)
    ld_wo = load(wo_h, wo)
    ld_og = load(og_h, og)

    barrier = pltpu.get_barrier_semaphore()
    peers = [{"y": lax.rem(y + o, ny)} for o in range(1, ny)]
    tps = [(o, t) for o in range(NX) for t in range(2) if (o, t) != (0, 0)]
    tp_peers = [{"x": lax.rem(x + o, NX), "c": lax.rem(c + t, 2)} for o, t in tps]
    peers += tp_peers
    for peer in peers:
        pl.semaphore_signal(barrier, inc=1, device_id=peer, device_id_type=MESH)
    later = nz - 1 - z
    group, place = lax.div(z, GROUP), lax.rem(z, GROUP)
    last = place == GROUP - 1
    reach = jnp.where(last, later, GROUP - 1 - place)

    def greet(d, carry):
        pl.semaphore_signal(barrier, inc=1, device_id={"z": z + d}, device_id_type=MESH)
        return carry

    lax.fori_loop(1, reach + 1, greet, 0)

    ld_ing.wait()

    def norm_rows(i, carry):
        at = pl.ds(pl.multiple_of(i * 16, 16), 16)
        wide = tok[at, :].astype(f32)
        scale = lax.rsqrt(jnp.mean(wide * wide, axis=1, keepdims=True) + norm_eps)
        nrm[at, :] = (wide * scale * ing[...]).astype(bf16)
        return carry

    tiles = part_rows // 16
    for i in range(TOKEN_PARTS):
        ld_tok[i].wait()
        lax.fori_loop(i * tiles, (i + 1) * tiles, norm_rows, 0, unroll=6)

    ld_dd.wait()
    ld_du.wait()
    ld_off.wait()
    ld_ext.wait()
    ld_wk.wait()
    ld_wv.wait()
    low = dot(nrm[...], dd[...], 1, 1).astype(bf16)
    kk[...] = dot(nrm[...], wk[...]).astype(bf16)
    pre = dot(low, du[...]) + doff[...]
    vv[...] = dot(nrm[...], wv[...]).astype(bf16)
    log_decay = (jnp.minimum(pre, 0.0) - jnp.log1p(jnp.exp(-jnp.abs(pre)))) / decay_temper + ext[...]
    d_hi = log_decay.astype(bf16)
    rest = log_decay - d_hi.astype(f32)
    d_mid = rest.astype(bf16)
    d_low = (rest - d_mid.astype(f32)).astype(bf16)
    size = (CHUNK, CHUNK)
    r_at, c_at = lax.broadcasted_iota(jnp.int32, size, 0), lax.broadcasted_iota(jnp.int32, size, 1)
    lower = jnp.where(r_at >= c_at, 1.0, 0.0).astype(bf16)
    carried = jnp.zeros((1, QUERY_FEATURES), f32)
    for i in range(chunks):
        own = slice(i * CHUNK, (i + 1) * CHUNK)
        sums = dot(lower, jnp.concatenate([d_hi[own], d_mid[own], d_low[own]], axis=1))
        sums = sums[:, :128] + (sums[:, 128:256] + sums[:, 256:]) + carried
        cum[own, :] = sums
        carried = sums[CHUNK - 1 :, :]
    closing = cum[rows - 1 : rows, :]
    gsend[...] = closing
    garr[y] = closing

    khat = (kk[...].astype(f32) * jnp.exp(closing - cum[...])).astype(bf16)
    state = dot(vv[...], khat, 0, 0).astype(bf16)
    st[...] = state.reshape(ny, piece, QUERY_FEATURES)
    arr[y] = st[y]

    def copy1(o):
        to = lax.rem(y + o, ny)
        return (
            pltpu.make_async_remote_copy(
                src_ref=st.at[to], dst_ref=arr.at[y], send_sem=s1s, recv_sem=s1r,
                device_id={"y": to}, device_id_type=MESH),
            pltpu.make_async_remote_copy(
                src_ref=gsend, dst_ref=garr.at[y], send_sem=g1s, recv_sem=g1r,
                device_id={"y": to}, device_id_type=MESH),
        )

    def all_of(ref, count, sem):
        some = ref.at[pl.ds(0, count)]
        pltpu.make_async_copy(some, some, sem).wait()

    pl.semaphore_wait(barrier, len(peers) + place + group)
    for o in far_first(ny):
        for copy in copy1(o):
            copy.start()

    def tell_near(d, carry):
        pl.semaphore_signal(ready.at[z], inc=1, device_id={"z": z - d}, device_id_type=MESH)
        return carry

    def tell_last(g, carry):
        pl.semaphore_signal(ready.at[z], inc=1, device_id={"z": g * GROUP + GROUP - 1}, device_id_type=MESH)
        return carry

    lax.fori_loop(1, place + 1, tell_near, 0)
    lax.fori_loop(0, group, tell_last, 0)

    ld_wq.wait()
    qq[...] = dot(nrm[...], wq[...]).astype(bf16)
    qhat[...] = (qq[...].astype(f32) * jnp.exp(cum[...])).astype(bf16)
    ld_wg.wait()
    ld_hg.wait()
    gate = dot(nrm[...], wg[...]).astype(bf16).astype(f32)
    fac[...] = gate * (1.0 / (1.0 + jnp.exp(-gate))) * hg[...]

    mid = CHUNK // 2
    same = (r_at >= c_at) & ((r_at >= mid) == (c_at >= mid))
    cross = (r_at >= mid) & (c_at < mid)
    for i in range(chunks):
        lo = i * CHUNK
        own = slice(lo, lo + CHUNK)
        q = qq[own, :].astype(f32)
        k = kk[own, :].astype(f32)
        at = cum[own, :]
        pivot = jnp.concatenate(
            [jnp.broadcast_to(cum[lo + j + mid // 2 - 1 : lo + j + mid // 2, :], (mid, QUERY_FEATURES)) for j in (0, mid)], axis=0)
        border = cum[lo + mid - 1 : lo + mid, :]
        near = dot_wide(q * jnp.exp(at - pivot), k * jnp.exp(pivot - at))
        step = dot_wide(q * jnp.exp(jnp.minimum(at - border, 0.0)), k * jnp.exp(jnp.minimum(border - at, 0.0)))
        scores = jnp.where(same, near, jnp.where(cross, step, 0.0)).astype(bf16)
        result = dot(scores, vv[own, :])
        if i:
            start = cum[lo - 1 : lo, :]
            before = slice(0, lo)
            earlier = dot_wide(
                q * jnp.exp(at - start), kk[before, :].astype(f32) * jnp.exp(start - cum[before, :]))
            result = result + dot(earlier.astype(bf16), vv[before, :])
        att[own, :] = result

    all_of(arr, ny - 1, s1r)
    all_of(garr, ny - 1, g1r)
    run = jnp.zeros((piece, QUERY_FEATURES), f32)
    total = jnp.zeros((1, QUERY_FEATURES), f32)
    for k in range(ny):
        inside[k] = run
        wbuf[k] = jnp.exp(total)
        run = jnp.exp(garr[k]) * run + arr[k].astype(f32)
        total = total + garr[k]
    tsend[0] = run.astype(bf16)
    gtsend[0] = total

    def copy2(level, d, slot, recv):
        send, land = (s2s, g2s), ((zarr, zgarr), (zfar, zgfar))[level]
        to = {"z": lax.rem(z + d, nz)}
        return [
            pltpu.make_async_remote_copy(
                src_ref=src.at[level], dst_ref=dst.at[slot], send_sem=sem.at[level], recv_sem=got.at[slot],
                device_id=to, device_id_type=MESH)
            for src, dst, sem, got in zip((tsend, gtsend), land, send, recv)
        ]

    def send_near(d, carry):
        pl.semaphore_wait(ready.at[z + d], 1)
        for copy in copy2(0, d, d, (s2r, g2r)):
            copy.start()
        return carry

    lax.fori_loop(1, GROUP - place, send_near, 0)

    def take_near(d, carry):
        into, weight = carry
        for copy in copy2(0, d, d, (s2r, g2r)):
            copy.wait_recv()
        return into + jnp.exp(weight) * zarr[d].astype(f32), weight + zgarr[d]

    nothing = (jnp.zeros((piece, QUERY_FEATURES), f32), jnp.zeros((1, QUERY_FEATURES), f32))
    near, near_weight = lax.fori_loop(1, place + 1, take_near, nothing)

    groups = nz // GROUP

    def send_far(g, carry):
        for p in range(GROUP):
            pl.semaphore_wait(ready.at[g * GROUP + p], 1)
            for copy in copy2(1, (g - group) * GROUP + p + 1 - GROUP, group, (s2f, g2f)):
                copy.start()
        return carry

    until = jnp.where(group == 0, 2, groups)

    @pl.when(last)
    def _():
        tsend[1] = (jnp.exp(total) * near + run).astype(bf16)
        gtsend[1] = near_weight + total

        lax.fori_loop(group + 1, until, send_far, 0)

    def take_far(i, carry):
        into, weight = carry
        g = group - 1 - i
        for copy in copy2(1, 1, g, (s2f, g2f)):
            copy.wait_recv()
        return into + jnp.exp(weight) * zfar[g].astype(f32), weight + zgfar[g]

    far, _ = lax.fori_loop(0, group, take_far, nothing)
    ahead = jnp.exp(near_weight) * far + near

    for k in range(ny):
        bsend[k] = (wbuf[k] * ahead + inside[k]).astype(bf16)

    first_of_all = (z == 0) & (y == 0)

    def copy3(o):
        to = lax.rem(y + o, ny)
        slot = y + jnp.where((z == 0) & (to == 0), ny, 0)
        return pltpu.make_async_remote_copy(
            src_ref=bsend.at[to], dst_ref=sin.at[slot], send_sem=s3s, recv_sem=s3r,
            device_id={"y": to}, device_id_type=MESH)

    for o in far_first(ny):
        copy3(o).start()

    @pl.when(last & (group == 0))
    def _():
        lax.fori_loop(until, groups, send_far, 0)

    @pl.when(first_of_all)
    def _():
        sin[pl.ds(0, ny)] = jnp.zeros((ny, piece, QUERY_FEATURES), bf16)

    @pl.when(jnp.logical_not(first_of_all))
    def _():
        sin[y] = bsend[y]
        all_of(sin, ny - 1, s3r)

    come = sin[pl.ds(0, ny)].reshape(DV, QUERY_FEATURES)

    first, second = pl.ds(0, half), pl.ds(half, half)
    quarters = [pl.ds(i * (half // 2), half // 2) for i in range(4)]

    def go(slot, part, k, where):
        return pltpu.make_async_remote_copy(
            src_ref=gat.at[slot, part], dst_ref=gat.at[slot, part], send_sem=gs.at[{0: 0, 14: 0, 2: 1, 15: 1}.get(k, 2)], recv_sem=gr.at[k],
            device_id=where, device_id_type=MESH)

    east, west, other = {"x": plus}, {"x": minus}, {"c": 1 - c}
    from_west, from_east, from_far = minus * 2 + c, plus * 2 + c, across * 2 + c
    twin = 1 - 2 * c

    for part, sends in ((first, ((0, 0, east), (1, 14, east))), (second, ((2, 2, west), (3, 15, west)))):
        there = att[part, :] + dot(qhat[part, :], come, 1, 1)
        scale = lax.rsqrt(jnp.mean(there * there, axis=1, keepdims=True) + norm_eps)
        gat[me, part, :] = (there * scale * fac[part, :]).astype(bf16)
        for i, k, where in sends:
            go(me, quarters[i], k, where).start()
    go(me, first, 6, other).start()
    go(me, second, 7, other).start()

    ld_wo.wait()

    def add(slot, part, fresh=False):
        term = dot(gat[slot, part, :], wo[pl.ds(pl.multiple_of(slot * DV, DV), DV), :])
        acc[part, :] = term if fresh else acc[part, :] + term

    add(me, first, True)
    add(me, second, True)
    all_of(gat.at[0], half, gs.at[0])
    go(me, second, 1, east).start()
    all_of(gat.at[0], half, gs.at[1])
    go(me, first, 3, west).start()

    def hand_on_east():
        for i, k, on in ((0, 0, 4), (1, 14, 16)):
            go(from_west, quarters[i], k, west).wait_recv()
            go(from_west, quarters[i], on, east).start()

    def hand_on_west():
        for i, k, on in ((2, 2, 5), (3, 15, 17)):
            go(from_east, quarters[i], k, east).wait_recv()
            go(from_east, quarters[i], on, west).start()

    @pl.when(x == 1)
    def _():
        hand_on_west()
        hand_on_east()

    @pl.when(x != 1)
    def _():
        hand_on_east()
        hand_on_west()

    go(from_west, first, 8, other).start()
    go(from_east, second, 9, other).start()
    go(me + twin, first, 6, other).wait_recv()
    go(me + twin, second, 7, other).wait_recv()
    add(me + twin, first)
    add(me + twin, second)
    add(from_west, first)
    add(from_east, second)
    go(from_west, second, 1, west).wait_recv()
    go(from_west, second, 10, other).start()
    go(from_east, first, 3, east).wait_recv()
    go(from_east, first, 11, other).start()
    add(from_west, second)
    add(from_east, first)
    go(from_west + twin, first, 8, other).wait_recv()
    add(from_west + twin, first)
    go(from_east + twin, second, 9, other).wait_recv()
    add(from_east + twin, second)
    go(from_west + twin, second, 10, other).wait_recv()
    add(from_west + twin, second)
    go(from_east + twin, first, 11, other).wait_recv()
    add(from_east + twin, first)
    go(from_far, quarters[0], 4, west).wait_recv()
    go(from_far, quarters[1], 16, west).wait_recv()
    go(from_far, first, 12, other).start()
    go(from_far, quarters[2], 5, east).wait_recv()
    go(from_far, quarters[3], 17, east).wait_recv()
    go(from_far, second, 13, other).start()
    add(from_far, first)
    add(from_far, second)
    go(from_far + twin, first, 12, other).wait_recv()
    add(from_far + twin, first)
    go(from_far + twin, second, 13, other).wait_recv()
    add(from_far + twin, second)

    mixed = acc[...]
    folded = mixed * mixed
    folded = folded[:, :128] + folded[:, 128:]
    ssend[...] = jnp.zeros_like(ssend)
    for i in range(chunks):
        flipped = folded[i * CHUNK : (i + 1) * CHUNK, :].T
        ssend[i : i + 1, :] = jnp.sum(flipped, axis=0, keepdims=True)

    def copy_ss(j):
        return pltpu.make_async_remote_copy(
            src_ref=ssend, dst_ref=sarr.at[me], send_sem=nss, recv_sem=nsr,
            device_id=tp_peers[j], device_id_type=MESH)

    for j in range(len(tps)):
        copy_ss(j).start()
    sarr[me] = ssend[...]
    ld_og.wait()
    all_of(sarr, len(tps), nsr)
    squares = sarr[0]
    for j in range(1, 2 * NX):
        squares = squares + sarr[j]
    inverse = lax.rsqrt(squares / (2 * NX * DV) + norm_eps)
    for i in range(chunks):
        own = slice(i * CHUNK, (i + 1) * CHUNK)
        per_row = jnp.broadcast_to(inverse[i : i + 1, :], size).T
        for j in range(0, DV, 128):
            out_ref[own, j : j + 128] = (acc[own, j : j + 128] * per_row * og[:, j : j + 128]).astype(out_ref.dtype)

    @pl.when(first_of_all)
    def _():
        all_of(sin, ny - 1, s3r)

    all_of(st, ny - 1, s1s)
    all_of(garr, ny - 1, g1s)
    all_of(bsend, ny - 1, s3s)
    all_of(sarr, len(tps), nss)

    for p in range(GROUP - 1):
        @pl.when(place == p)
        def _(count=GROUP - 1 - p):
            all_of(zfar, count, s2s.at[0])
            all_of(zgfar, count, g2s.at[0])

    for g in range(nz // GROUP - 1):
        @pl.when(last & (group == g))
        def _(count=nz - GROUP * (g + 1)):
            all_of(zfar, count, s2s.at[1])
            all_of(zgfar, count, g2s.at[1])

    all_of(gat, 6, gs.at[2])


def local(nz, ny, *args):
    (tokens, in_gain, query_weight, key_weight, value_weight, gate_weight, decay_down, decay_up,
     decay_offset, decay_extra, head_gain, out_weight, out_gain) = args
    rows, width = tokens.shape
    piece = DV // ny
    rank = decay_down.shape[1]
    in_hbm = pl.BlockSpec(memory_space=pltpu.HBM)
    dma = pltpu.SemaphoreType.DMA
    V = pltpu.VMEM
    scratch = [
        V((rows, width), bf16),
        V((rows, width), bf16),
        V((width, QUERY_FEATURES), bf16),
        V((width, QUERY_FEATURES), bf16),
        V((width, DV), bf16),
        V((width, DV), bf16),
        V((2 * NX * DV, DV), bf16),
        V((rank, width), bf16),
        V((rank, QUERY_FEATURES), bf16),
        V((1, width), f32),
        V((1, QUERY_FEATURES), f32),
        V((rows, QUERY_FEATURES), f32),
        V((1, DV), f32),
        V((1, DV), f32),
        V((rows, QUERY_FEATURES), f32),
        V((rows, QUERY_FEATURES), bf16),
        V((rows, DV), bf16),
        V((rows, QUERY_FEATURES), bf16),
        V((rows, DV), f32),
        V((rows, QUERY_FEATURES), bf16),
        V((rows, DV), f32),
        V((ny, piece, QUERY_FEATURES), bf16),
        V((1, QUERY_FEATURES), f32),
        V((ny, piece, QUERY_FEATURES), bf16),
        V((ny, 1, QUERY_FEATURES), f32),
        V((ny, piece, QUERY_FEATURES), f32),
        V((ny, 1, QUERY_FEATURES), f32),
        V((2, piece, QUERY_FEATURES), bf16),
        V((2, 1, QUERY_FEATURES), f32),
        V((GROUP, piece, QUERY_FEATURES), bf16),
        V((GROUP, 1, QUERY_FEATURES), f32),
        V((nz, piece, QUERY_FEATURES), bf16),
        V((nz, 1, QUERY_FEATURES), f32),
        V((ny, piece, QUERY_FEATURES), bf16),
        V((2 * ny, piece, QUERY_FEATURES), bf16),
        V((2 * NX, rows, DV), bf16),
        V((rows, DV), f32),
        V((8, 128), f32),
        V((2 * NX, 8, 128), f32),
        pltpu.SemaphoreType.REGULAR((nz,)),
        dma((12 + TOKEN_PARTS,)),
        dma, dma, dma, dma,
        dma((2,)), dma((GROUP,)), dma((2,)), dma((GROUP,)), dma((nz // GROUP,)), dma((nz // GROUP,)),
        dma, dma,
        dma((3,)), dma((18,)),
        dma, dma,
    ]
    operands = (
        tokens, in_gain.reshape(1, -1), query_weight, key_weight, value_weight, gate_weight, decay_down.T, decay_up,
        decay_offset.reshape(1, -1), decay_extra, head_gain.reshape(1, -1), out_weight, out_gain.reshape(1, -1),
    )
    return pl.pallas_call(
        functools.partial(kernel, nz, ny),
        out_shape=jax.ShapeDtypeStruct((rows, DV), bf16),
        in_specs=[in_hbm] * 13,
        out_specs=pl.BlockSpec(memory_space=pltpu.VMEM),
        scratch_shapes=scratch,
        compiler_params=pltpu.CompilerParams(collective_id=0, has_side_effects=True, vmem_limit_bytes=48 << 20),
        name="linear_attention",
    )(*(pltpu.with_memory_space_constraint(operand, pltpu.HBM) for operand in operands))


def build(devices, nz, ny):
    torus = Mesh(devices.reshape(nz, ny, NX, 2), ("z", "y", "x", "c"))
    sp, tp = ("z", "y"), ("x", "c")
    in_specs = (
        P(sp, None), P(), P(None, tp), P(None, tp), P(None, tp), P(None, tp), P(), P(), P(tp),
        P(sp, tp), P(tp), P(None, tp), P(tp),
    )
    return jax.shard_map(
        functools.partial(local, nz, ny), mesh=torus, in_specs=in_specs, out_specs=P(sp, tp), check_vma=False)


def solution(mesh):
    ny = 8
    return build(mesh.devices, mesh.shape["sp"] // ny, ny)
```

```python
import functools

import jax
import jax.numpy as jnp
from jax import lax
from jax.experimental import pallas as pl
from jax.experimental.pallas import tpu as pltpu
from jax.sharding import Mesh
from jax.sharding import PartitionSpec as P

QUERY_FEATURES = 128
DV = 256
CHUNK = 128
TOKEN_PARTS = 4
GROUP = 4
NX = 4
norm_eps = 1e-06
decay_temper = 16.0
MESH = pl.DeviceIdType.MESH
f32 = jnp.float32
bf16 = jnp.bfloat16


def dot(a, b, ca=1, cb=0):
    return lax.dot_general(a, b, (((ca,), (cb,)), ((), ())), preferred_element_type=f32)


def dot_wide(a, b):
    a_hi, b_hi = a.astype(bf16), b.astype(bf16)
    a_lo, b_lo = (a - a_hi.astype(f32)).astype(bf16), (b - b_hi.astype(f32)).astype(bf16)
    return dot(jnp.concatenate([a_hi, a_hi, a_lo], axis=1), jnp.concatenate([b_hi, b_lo, b_hi], axis=1), 1, 1)


def far_first(n):
    return sorted(range(1, n), key=lambda o: -min(o, n - o))


def kernel(
    nz,
    ny,
    tok_h,
    ing_h,
    wq_h,
    wk_h,
    wv_h,
    wg_h,
    dd_h,
    du_h,
    off_h,
    ext_h,
    hg_h,
    wo_h,
    og_h,
    out_ref,
    tok,
    nrm,
    wq,
    wk,
    wv,
    wg,
    wo,
    dd,
    du,
    ing,
    doff,
    ext,
    hg,
    og,
    cum,
    kk,
    vv,
    qq,
    fac,
    qhat,
    att,
    st,
    gsend,
    arr,
    garr,
    inside,
    wbuf,
    tsend,
    gtsend,
    zarr,
    zgarr,
    zfar,
    zgfar,
    bsend,
    sin,
    gat,
    acc,
    ssend,
    sarr,
    ready,
    lsem,
    s1s,
    s1r,
    g1s,
    g1r,
    s2s,
    s2r,
    g2s,
    g2r,
    s2f,
    g2f,
    s3s,
    s3r,
    gs,
    gr,
    nss,
    nsr,
):
    z, y, x, c = (lax.axis_index(name) for name in ("z", "y", "x", "c"))
    rows, width = tok.shape
    half = rows // 2
    chunks = rows // CHUNK
    piece = DV // ny
    me = x * 2 + c
    plus, minus, across = lax.rem(x + 1, NX), lax.rem(x + NX - 1, NX), lax.rem(x + 2, NX)

    loads = []

    def load(src, dst):
        copy = pltpu.make_async_copy(src, dst, lsem.at[len(loads)])
        copy.start()
        loads.append(copy)
        return copy

    part_rows = rows // TOKEN_PARTS
    ld_tok = [
        load(tok_h.at[pl.ds(i * part_rows, part_rows)], tok.at[pl.ds(i * part_rows, part_rows)])
        for i in range(TOKEN_PARTS)
    ]
    ld_ing = load(ing_h, ing)
    ld_dd = load(dd_h, dd)
    ld_du = load(du_h.at[:, pl.ds(pl.multiple_of(me * QUERY_FEATURES, QUERY_FEATURES), QUERY_FEATURES)], du)
    ld_off = load(off_h, doff)
    ld_ext = load(ext_h, ext)
    ld_wk = load(wk_h, wk)
    ld_wv = load(wv_h, wv)
    ld_wq = load(wq_h, wq)
    ld_wg = load(wg_h, wg)
    ld_hg = load(hg_h, hg)
    ld_wo = load(wo_h, wo)
    ld_og = load(og_h, og)

    barrier = pltpu.get_barrier_semaphore()
    peers = [{"y": lax.rem(y + o, ny)} for o in range(1, ny)]
    tps = [(o, t) for o in range(NX) for t in range(2) if (o, t) != (0, 0)]
    tp_peers = [{"x": lax.rem(x + o, NX), "c": lax.rem(c + t, 2)} for o, t in tps]
    peers += tp_peers
    for peer in peers:
        pl.semaphore_signal(barrier, inc=1, device_id=peer, device_id_type=MESH)
    later = nz - 1 - z
    group, place = lax.div(z, GROUP), lax.rem(z, GROUP)
    last = place == GROUP - 1
    reach = jnp.where(last, later, GROUP - 1 - place)

    def greet(d, carry):
        pl.semaphore_signal(barrier, inc=1, device_id={"z": z + d}, device_id_type=MESH)
        return carry

    lax.fori_loop(1, reach + 1, greet, 0)

    ld_ing.wait()

    def norm_rows(i, carry):
        at = pl.ds(pl.multiple_of(i * 16, 16), 16)
        wide = tok[at, :].astype(f32)
        scale = lax.rsqrt(jnp.mean(wide * wide, axis=1, keepdims=True) + norm_eps)
        nrm[at, :] = (wide * scale * ing[...]).astype(bf16)
        return carry

    tiles = part_rows // 16
    for i in range(TOKEN_PARTS):
        ld_tok[i].wait()
        lax.fori_loop(i * tiles, (i + 1) * tiles, norm_rows, 0, unroll=6)

    ld_dd.wait()
    ld_du.wait()
    ld_off.wait()
    ld_ext.wait()
    ld_wk.wait()
    ld_wv.wait()
    low = dot(nrm[...], dd[...], 1, 1).astype(bf16)
    kk[...] = dot(nrm[...], wk[...]).astype(bf16)
    pre = dot(low, du[...]) + doff[...]
    vv[...] = dot(nrm[...], wv[...]).astype(bf16)
    log_decay = (jnp.minimum(pre, 0.0) - jnp.log1p(jnp.exp(-jnp.abs(pre)))) / decay_temper + ext[...]
    d_hi = log_decay.astype(bf16)
    rest = log_decay - d_hi.astype(f32)
    d_mid = rest.astype(bf16)
    d_low = (rest - d_mid.astype(f32)).astype(bf16)
    size = (CHUNK, CHUNK)
    r_at, c_at = lax.broadcasted_iota(jnp.int32, size, 0), lax.broadcasted_iota(jnp.int32, size, 1)
    lower = jnp.where(r_at >= c_at, 1.0, 0.0).astype(bf16)
    carried = jnp.zeros((1, QUERY_FEATURES), f32)
    for i in range(chunks):
        own = slice(i * CHUNK, (i + 1) * CHUNK)
        sums = dot(lower, jnp.concatenate([d_hi[own], d_mid[own], d_low[own]], axis=1))
        sums = sums[:, :128] + (sums[:, 128:256] + sums[:, 256:]) + carried
        cum[own, :] = sums
        carried = sums[CHUNK - 1 :, :]
    closing = cum[rows - 1 : rows, :]
    gsend[...] = closing
    garr[y] = closing

    khat = (kk[...].astype(f32) * jnp.exp(closing - cum[...])).astype(bf16)
    state = dot(vv[...], khat, 0, 0).astype(bf16)
    st[...] = state.reshape(ny, piece, QUERY_FEATURES)
    arr[y] = st[y]

    def copy1(o):
        to = lax.rem(y + o, ny)
        return (
            pltpu.make_async_remote_copy(
                src_ref=st.at[to], dst_ref=arr.at[y], send_sem=s1s, recv_sem=s1r,
                device_id={"y": to}, device_id_type=MESH),
            pltpu.make_async_remote_copy(
                src_ref=gsend, dst_ref=garr.at[y], send_sem=g1s, recv_sem=g1r,
                device_id={"y": to}, device_id_type=MESH),
        )

    def all_of(ref, count, sem):
        some = ref.at[pl.ds(0, count)]
        pltpu.make_async_copy(some, some, sem).wait()

    pl.semaphore_wait(barrier, len(peers) + place + group)
    for o in far_first(ny):
        for copy in copy1(o):
            copy.start()

    def tell_near(d, carry):
        pl.semaphore_signal(ready.at[z], inc=1, device_id={"z": z - d}, device_id_type=MESH)
        return carry

    def tell_last(g, carry):
        pl.semaphore_signal(ready.at[z], inc=1, device_id={"z": g * GROUP + GROUP - 1}, device_id_type=MESH)
        return carry

    lax.fori_loop(1, place + 1, tell_near, 0)
    lax.fori_loop(0, group, tell_last, 0)

    ld_wq.wait()
    qq[...] = dot(nrm[...], wq[...]).astype(bf16)
    qhat[...] = (qq[...].astype(f32) * jnp.exp(cum[...])).astype(bf16)
    ld_wg.wait()
    ld_hg.wait()
    gate = dot(nrm[...], wg[...]).astype(bf16).astype(f32)
    fac[...] = gate * (1.0 / (1.0 + jnp.exp(-gate))) * hg[...]

    mid = CHUNK // 2
    same = (r_at >= c_at) & ((r_at >= mid) == (c_at >= mid))
    cross = (r_at >= mid) & (c_at < mid)
    for i in range(chunks):
        lo = i * CHUNK
        own = slice(lo, lo + CHUNK)
        q = qq[own, :].astype(f32)
        k = kk[own, :].astype(f32)
        at = cum[own, :]
        pivot = jnp.concatenate(
            [jnp.broadcast_to(cum[lo + j + mid // 2 - 1 : lo + j + mid // 2, :], (mid, QUERY_FEATURES)) for j in (0, mid)], axis=0)
        border = cum[lo + mid - 1 : lo + mid, :]
        near = dot_wide(q * jnp.exp(at - pivot), k * jnp.exp(pivot - at))
        step = dot_wide(q * jnp.exp(jnp.minimum(at - border, 0.0)), k * jnp.exp(jnp.minimum(border - at, 0.0)))
        scores = jnp.where(same, near, jnp.where(cross, step, 0.0)).astype(bf16)
        result = dot(scores, vv[own, :])
        if i:
            start = cum[lo - 1 : lo, :]
            before = slice(0, lo)
            earlier = dot_wide(
                q * jnp.exp(at - start), kk[before, :].astype(f32) * jnp.exp(start - cum[before, :]))
            result = result + dot(earlier.astype(bf16), vv[before, :])
        att[own, :] = result

    all_of(arr, ny - 1, s1r)
    all_of(garr, ny - 1, g1r)
    run = jnp.zeros((piece, QUERY_FEATURES), f32)
    total = jnp.zeros((1, QUERY_FEATURES), f32)
    for k in range(ny):
        inside[k] = run
        wbuf[k] = jnp.exp(total)
        run = jnp.exp(garr[k]) * run + arr[k].astype(f32)
        total = total + garr[k]
    tsend[0] = run.astype(bf16)
    gtsend[0] = total

    def copy2(level, d, slot, recv):
        send, land = (s2s, g2s), ((zarr, zgarr), (zfar, zgfar))[level]
        to = {"z": lax.rem(z + d, nz)}
        return [
            pltpu.make_async_remote_copy(
                src_ref=src.at[level], dst_ref=dst.at[slot], send_sem=sem.at[level], recv_sem=got.at[slot],
                device_id=to, device_id_type=MESH)
            for src, dst, sem, got in zip((tsend, gtsend), land, send, recv)
        ]

    def send_near(d, carry):
        pl.semaphore_wait(ready.at[z + d], 1)
        for copy in copy2(0, d, d, (s2r, g2r)):
            copy.start()
        return carry

    lax.fori_loop(1, GROUP - place, send_near, 0)

    def take_near(d, carry):
        into, weight = carry
        for copy in copy2(0, d, d, (s2r, g2r)):
            copy.wait_recv()
        return into + jnp.exp(weight) * zarr[d].astype(f32), weight + zgarr[d]

    nothing = (jnp.zeros((piece, QUERY_FEATURES), f32), jnp.zeros((1, QUERY_FEATURES), f32))
    near, near_weight = lax.fori_loop(1, place + 1, take_near, nothing)

    groups = nz // GROUP

    def send_far(g, carry):
        for p in range(GROUP):
            pl.semaphore_wait(ready.at[g * GROUP + p], 1)
            for copy in copy2(1, (g - group) * GROUP + p + 1 - GROUP, group, (s2f, g2f)):
                copy.start()
        return carry

    until = jnp.where(group == 0, 2, groups)

    @pl.when(last)
    def _():
        tsend[1] = (jnp.exp(total) * near + run).astype(bf16)
        gtsend[1] = near_weight + total

        lax.fori_loop(group + 1, until, send_far, 0)

    def take_far(i, carry):
        into, weight = carry
        g = group - 1 - i
        for copy in copy2(1, 1, g, (s2f, g2f)):
            copy.wait_recv()
        return into + jnp.exp(weight) * zfar[g].astype(f32), weight + zgfar[g]

    far, _ = lax.fori_loop(0, group, take_far, nothing)
    ahead = jnp.exp(near_weight) * far + near

    for k in range(ny):
        bsend[k] = (wbuf[k] * ahead + inside[k]).astype(bf16)

    first_of_all = (z == 0) & (y == 0)

    def copy3(o):
        to = lax.rem(y + o, ny)
        slot = y + jnp.where((z == 0) & (to == 0), ny, 0)
        return pltpu.make_async_remote_copy(
            src_ref=bsend.at[to], dst_ref=sin.at[slot], send_sem=s3s, recv_sem=s3r,
            device_id={"y": to}, device_id_type=MESH)

    for o in far_first(ny):
        copy3(o).start()

    @pl.when(last & (group == 0))
    def _():
        lax.fori_loop(until, groups, send_far, 0)

    @pl.when(first_of_all)
    def _():
        sin[pl.ds(0, ny)] = jnp.zeros((ny, piece, QUERY_FEATURES), bf16)

    @pl.when(jnp.logical_not(first_of_all))
    def _():
        sin[y] = bsend[y]
        all_of(sin, ny - 1, s3r)

    come = sin[pl.ds(0, ny)].reshape(DV, QUERY_FEATURES)

    first, second = pl.ds(0, half), pl.ds(half, half)
    quarters = [pl.ds(i * (half // 2), half // 2) for i in range(4)]

    def go(slot, part, k, where):
        return pltpu.make_async_remote_copy(
            src_ref=gat.at[slot, part], dst_ref=gat.at[slot, part], send_sem=gs.at[0 if k in (6, 7) else 1], recv_sem=gr.at[k],
            device_id=where, device_id_type=MESH)

    east, west, other = {"x": plus}, {"x": minus}, {"c": 1 - c}
    from_west, from_east, from_far = minus * 2 + c, plus * 2 + c, across * 2 + c
    twin = 1 - 2 * c

    for part, sends in ((first, ((0, 0, east), (1, 14, east))), (second, ((2, 2, west), (3, 15, west)))):
        there = att[part, :] + dot(qhat[part, :], come, 1, 1)
        scale = lax.rsqrt(jnp.mean(there * there, axis=1, keepdims=True) + norm_eps)
        gat[me, part, :] = (there * scale * fac[part, :]).astype(bf16)
        for i, k, where in sends:
            go(me, quarters[i], k, where).start()
    go(me, first, 6, other).start()
    go(me, second, 7, other).start()

    ld_wo.wait()

    def add(slot, part, fresh=False):
        term = dot(gat[slot, part, :], wo[pl.ds(pl.multiple_of(slot * DV, DV), DV), :])
        acc[part, :] = term if fresh else acc[part, :] + term

    add(me, first, True)
    add(me, second, True)
    all_of(gat.at[0], rows, gs.at[0])
    go(me, second, 1, east).start()
    go(me, first, 3, west).start()

    def hand_on_east():
        for i, k, on in ((0, 0, 4), (1, 14, 16)):
            go(from_west, quarters[i], k, west).wait_recv()
            go(from_west, quarters[i], on, east).start()

    def hand_on_west():
        for i, k, on in ((2, 2, 5), (3, 15, 17)):
            go(from_east, quarters[i], k, east).wait_recv()
            go(from_east, quarters[i], on, west).start()

    @pl.when(x == 1)
    def _():
        hand_on_west()
        hand_on_east()

    @pl.when(x != 1)
    def _():
        hand_on_east()
        hand_on_west()

    go(from_west, first, 8, other).start()
    go(from_east, second, 9, other).start()
    add(from_west, first)
    add(from_east, second)
    go(from_west, second, 1, west).wait_recv()
    go(from_west, second, 10, other).start()
    go(from_east, first, 3, east).wait_recv()
    go(from_east, first, 11, other).start()
    add(from_west, second)
    add(from_east, first)
    go(from_far, quarters[0], 4, west).wait_recv()
    go(from_far, quarters[1], 16, west).wait_recv()
    go(from_far, first, 12, other).start()
    go(from_far, quarters[2], 5, east).wait_recv()
    go(from_far, quarters[3], 17, east).wait_recv()
    go(from_far, second, 13, other).start()
    for slot, part, k in (
        (me, first, 6), (me, second, 7), (from_west, first, 8), (from_east, second, 9),
        (from_west, second, 10), (from_east, first, 11),
    ):
        go(slot + twin, part, k, other).wait_recv()
        add(slot + twin, part)
    add(from_far, first)
    add(from_far, second)
    go(from_far + twin, first, 12, other).wait_recv()
    add(from_far + twin, first)
    go(from_far + twin, second, 13, other).wait_recv()
    add(from_far + twin, second)

    mixed = acc[...]
    folded = mixed * mixed
    folded = folded[:, :128] + folded[:, 128:]
    ssend[...] = jnp.zeros_like(ssend)
    for i in range(chunks):
        flipped = folded[i * CHUNK : (i + 1) * CHUNK, :].T
        ssend[i : i + 1, :] = jnp.sum(flipped, axis=0, keepdims=True)

    def copy_ss(j):
        return pltpu.make_async_remote_copy(
            src_ref=ssend, dst_ref=sarr.at[me], send_sem=nss, recv_sem=nsr,
            device_id=tp_peers[j], device_id_type=MESH)

    for j in range(len(tps)):
        copy_ss(j).start()
    sarr[me] = ssend[...]
    ld_og.wait()
    all_of(sarr, len(tps), nsr)
    squares = sarr[0]
    for j in range(1, 2 * NX):
        squares = squares + sarr[j]
    inverse = lax.rsqrt(squares / (2 * NX * DV) + norm_eps)
    for i in range(chunks):
        own = slice(i * CHUNK, (i + 1) * CHUNK)
        per_row = jnp.broadcast_to(inverse[i : i + 1, :], size).T
        for j in range(0, DV, 128):
            out_ref[own, j : j + 128] = (acc[own, j : j + 128] * per_row * og[:, j : j + 128]).astype(out_ref.dtype)

    @pl.when(first_of_all)
    def _():
        all_of(sin, ny - 1, s3r)

    all_of(st, ny - 1, s1s)
    all_of(garr, ny - 1, g1s)
    all_of(bsend, ny - 1, s3s)
    all_of(sarr, len(tps), nss)

    for p in range(GROUP - 1):
        @pl.when(place == p)
        def _(count=GROUP - 1 - p):
            all_of(zfar, count, s2s.at[0])
            all_of(zgfar, count, g2s.at[0])

    for g in range(nz // GROUP - 1):
        @pl.when(last & (group == g))
        def _(count=nz - GROUP * (g + 1)):
            all_of(zfar, count, s2s.at[1])
            all_of(zgfar, count, g2s.at[1])

    all_of(gat, 6, gs.at[1])


def local(nz, ny, *args):
    (tokens, in_gain, query_weight, key_weight, value_weight, gate_weight, decay_down, decay_up,
     decay_offset, decay_extra, head_gain, out_weight, out_gain) = args
    rows, width = tokens.shape
    piece = DV // ny
    rank = decay_down.shape[1]
    in_hbm = pl.BlockSpec(memory_space=pltpu.HBM)
    dma = pltpu.SemaphoreType.DMA
    V = pltpu.VMEM
    scratch = [
        V((rows, width), bf16),
        V((rows, width), bf16),
        V((width, QUERY_FEATURES), bf16),
        V((width, QUERY_FEATURES), bf16),
        V((width, DV), bf16),
        V((width, DV), bf16),
        V((2 * NX * DV, DV), bf16),
        V((rank, width), bf16),
        V((rank, QUERY_FEATURES), bf16),
        V((1, width), f32),
        V((1, QUERY_FEATURES), f32),
        V((rows, QUERY_FEATURES), f32),
        V((1, DV), f32),
        V((1, DV), f32),
        V((rows, QUERY_FEATURES), f32),
        V((rows, QUERY_FEATURES), bf16),
        V((rows, DV), bf16),
        V((rows, QUERY_FEATURES), bf16),
        V((rows, DV), f32),
        V((rows, QUERY_FEATURES), bf16),
        V((rows, DV), f32),
        V((ny, piece, QUERY_FEATURES), bf16),
        V((1, QUERY_FEATURES), f32),
        V((ny, piece, QUERY_FEATURES), bf16),
        V((ny, 1, QUERY_FEATURES), f32),
        V((ny, piece, QUERY_FEATURES), f32),
        V((ny, 1, QUERY_FEATURES), f32),
        V((2, piece, QUERY_FEATURES), bf16),
        V((2, 1, QUERY_FEATURES), f32),
        V((GROUP, piece, QUERY_FEATURES), bf16),
        V((GROUP, 1, QUERY_FEATURES), f32),
        V((nz, piece, QUERY_FEATURES), bf16),
        V((nz, 1, QUERY_FEATURES), f32),
        V((ny, piece, QUERY_FEATURES), bf16),
        V((2 * ny, piece, QUERY_FEATURES), bf16),
        V((2 * NX, rows, DV), bf16),
        V((rows, DV), f32),
        V((8, 128), f32),
        V((2 * NX, 8, 128), f32),
        pltpu.SemaphoreType.REGULAR((nz,)),
        dma((12 + TOKEN_PARTS,)),
        dma, dma, dma, dma,
        dma((2,)), dma((GROUP,)), dma((2,)), dma((GROUP,)), dma((nz // GROUP,)), dma((nz // GROUP,)),
        dma, dma,
        dma((2,)), dma((18,)),
        dma, dma,
    ]
    operands = (
        tokens, in_gain.reshape(1, -1), query_weight, key_weight, value_weight, gate_weight, decay_down.T, decay_up,
        decay_offset.reshape(1, -1), decay_extra, head_gain.reshape(1, -1), out_weight, out_gain.reshape(1, -1),
    )
    return pl.pallas_call(
        functools.partial(kernel, nz, ny),
        out_shape=jax.ShapeDtypeStruct((rows, DV), bf16),
        in_specs=[in_hbm] * 13,
        out_specs=pl.BlockSpec(memory_space=pltpu.VMEM),
        scratch_shapes=scratch,
        compiler_params=pltpu.CompilerParams(collective_id=0, has_side_effects=True, vmem_limit_bytes=48 << 20),
        name="linear_attention",
    )(*(pltpu.with_memory_space_constraint(operand, pltpu.HBM) for operand in operands))


def build(devices, nz, ny):
    torus = Mesh(devices.reshape(nz, ny, NX, 2), ("z", "y", "x", "c"))
    sp, tp = ("z", "y"), ("x", "c")
    in_specs = (
        P(sp, None), P(), P(None, tp), P(None, tp), P(None, tp), P(None, tp), P(), P(), P(tp),
        P(sp, tp), P(tp), P(None, tp), P(tp),
    )
    return jax.shard_map(
        functools.partial(local, nz, ny), mesh=torus, in_specs=in_specs, out_specs=P(sp, tp), check_vma=False)


def solution(mesh):
    ny = 8
    return build(mesh.devices, mesh.shape["sp"] // ny, ny)
```
